32 devices in a mesh: ep: 8 (over z, x), tp: 4 (over y, core).
Axes of the slice: x: 2, y: 2, z: 4, core: 2. Of those that a mesh axis runs over, the one named last changes fastest.
Arguments:
- queries: bfloat16 [3072, 2048], P('ep', 'tp'), may hold values from -8 to 8
- keys: bfloat16 [3072, 2048], P('ep', 'tp'), may hold values from -8 to 8
- values: bfloat16 [3072, 2048], P('ep', 'tp'), may hold values from -6 to 6
- key_offset: bfloat16 [3072, 16], P('ep', 'tp'), may hold values from -15.25 to -0.4
- rows: bfloat16 [1024, 2048], P('ep'), may hold values from -6 to 6
- gain: float32 [2048], replicated, may hold values from 0.1 to 1.9
- gate_w: bfloat16 [8, 2048, 3584], P('ep', None, 'tp'), may hold values from -0.125 to 0.125
- up_w: bfloat16 [8, 2048, 3584], P('ep', None, 'tp'), may hold values from -0.125 to 0.125
- down_w: bfloat16 [8, 3584, 2048], P('ep', 'tp'), may hold values from -0.09375 to 0.09375
- expert_ids: int32 [1024, 2], P('ep'), may hold values from 0 to 7, all different within a row; in each aligned block of 128 rows (0 to 127, 128 to 255, ...) at most 64 rows name the same one
- route_weights: float32 [1024, 2], P('ep'), may hold values from 0.2 to 1
Outputs:
- attended: bfloat16 [3072, 2048], P('ep', 'tp')
- mixed: bfloat16 [1024, 2048], P('ep')
The draws below stay inside these ranges and needn't reach their ends.
Inputs may be any that keep to these rules, and one draw needn't show every extreme that they name: `expert_ids`: each token names 2 different experts; among the 128 tokens of one ep index no expert is chosen more than 64 times, and in some such block an expert is chosen exactly 64 times.
All inputs are finite; a program needn't handle non-finite values.
Results may differ from the reference program's by a relative error of at most 0.019.
Values may be sent and summed in bfloat16 or wider, within the bound.
A program may use at most 128 MiB of HBM per device.

```python
import math
import jax
import jax.numpy as jnp
import numpy as np
from jax import lax

D = 2048
ATTENTION_HEADS = 16
HD = 128
FF = 3584
TOP = 2
TOK_A_DEV = 384
TOK_B_DEV = 128
EXPERTS = 8
SEQUENCE_TOKENS = 3072
TOKENS_B = 1024
CAP = 64
N_TP = 4


def unit_noise(noise_key, shape):
    return jax.random.normal(noise_key, shape, jnp.float32)


def stick_fields(key):
    groups = 16
    center_key, value_key, query_id_key, key_id_key, query_amp_key, key_amp_key, query_noise_key, key_noise_key, value_noise_key = jax.random.split(jax.random.fold_in(key, 23), 9)
    centers = jax.random.normal(center_key, (ATTENTION_HEADS, groups, HD), jnp.float32)
    centers = centers / jnp.sqrt(jnp.sum(centers * centers, axis=2, keepdims=True))
    value_centers = jax.random.normal(value_key, (ATTENTION_HEADS, groups, HD), jnp.float32)
    strength = (5.0 * HD ** 0.5) ** 0.5
    head_index = jnp.arange(ATTENTION_HEADS, dtype=jnp.int32)[None, :]
    query_group = jax.random.randint(query_id_key, (SEQUENCE_TOKENS, ATTENTION_HEADS), 0, groups)
    key_group = jax.random.randint(key_id_key, (SEQUENCE_TOKENS, ATTENTION_HEADS), 0, groups)
    query_amplitude = jax.random.uniform(query_amp_key, (SEQUENCE_TOKENS, ATTENTION_HEADS, 1), jnp.float32, 0.8, 1.2)
    key_amplitude = jax.random.uniform(key_amp_key, (SEQUENCE_TOKENS, ATTENTION_HEADS, 1), jnp.float32, 0.8, 1.2)
    shape = (SEQUENCE_TOKENS, ATTENTION_HEADS, HD)
    query_field = 1.2 * unit_noise(query_noise_key, shape) + strength * query_amplitude * centers[head_index, query_group]
    key_field = 1.2 * unit_noise(key_noise_key, shape) + strength * key_amplitude * centers[head_index, key_group]
    value_field = 0.6 * unit_noise(value_noise_key, shape) + 0.8 * value_centers[head_index, key_group]
    query_field = jnp.clip(query_field.reshape(SEQUENCE_TOKENS, ATTENTION_HEADS * HD), -8.0, 8.0)
    key_field = jnp.clip(key_field.reshape(SEQUENCE_TOKENS, ATTENTION_HEADS * HD), -8.0, 8.0)
    value_field = jnp.clip(value_field.reshape(SEQUENCE_TOKENS, ATTENTION_HEADS * HD), -6.0, 6.0)
    return (query_field, key_field, value_field)


def draw_queries(key, part):
    return stick_fields(key)[0].astype(jnp.bfloat16)


def draw_keys(key, part):
    return stick_fields(key)[1].astype(jnp.bfloat16)


def draw_values(key, part):
    return stick_fields(key)[2].astype(jnp.bfloat16)


def draw_key_offset(key, part):
    select_random_key, quick_random_key, gradual_random_key, offset_random_key, noise_random_key, spike_random_key, height_random_key = jax.random.split(jax.random.fold_in(key, 11), 7)
    slow_base = jax.random.uniform(gradual_random_key, (ATTENTION_HEADS,), jnp.float32, -14.0, -12.5)
    fast_base = jax.random.uniform(quick_random_key, (ATTENTION_HEADS,), jnp.float32, -8.0, -7.0)
    chosen = jax.random.uniform(select_random_key, (ATTENTION_HEADS,), jnp.float32) < 0.5
    base = jnp.where(chosen, fast_base, slow_base)
    blocks = SEQUENCE_TOKENS // TOK_A_DEV
    shift = jax.random.uniform(offset_random_key, (blocks, 1, ATTENTION_HEADS), jnp.float32, -0.7, 0.7)
    jitter = jax.random.uniform(noise_random_key, (blocks, TOK_A_DEV, ATTENTION_HEADS), jnp.float32, -0.5, 0.5)
    base_height = (base[None, None, :] + shift + jitter).reshape(SEQUENCE_TOKENS, ATTENTION_HEADS)
    spike_amount = jax.random.uniform(spike_random_key, (SEQUENCE_TOKENS, ATTENTION_HEADS), jnp.float32) < 8.0 / SEQUENCE_TOKENS
    spike_height = jax.random.uniform(height_random_key, (SEQUENCE_TOKENS, ATTENTION_HEADS), jnp.float32, -1.2, -0.4)
    return jnp.where(spike_amount, spike_height, base_height).astype(jnp.bfloat16)


def levels(stream_key, shape, cuts, low, largest):
    def one(axis_at, shards_of):
        heights = jax.random.uniform(jax.random.fold_in(jax.random.fold_in(stream_key, 6), axis_at), (shards_of,), jnp.float32, low / len(cuts), largest / len(cuts))
        return jnp.repeat(jnp.exp(heights), shape[axis_at] // shards_of).reshape((-1,) + (1,) * (len(shape) - axis_at - 1))

    loudness = one(*cuts[0])
    for cut in cuts[1:]:
        loudness = loudness * one(*cut)
    return loudness


def deal_out(key, own, number, rows, count, top, limit, skew):
    ranking = jax.random.permutation(key, count)
    crowded, ordinary = shares(count, rows * top, limit, skew, True), shares(count, rows * top, limit, skew, False)
    places = jnp.arange(count)

    def named(lengths, offset_by):
        used = int((lengths > 0).sum())
        fixed = max(1, used // 4)
        shifted = fixed + (places - fixed + offset_by * (used - fixed)) % max(1, count - fixed)
        return jnp.zeros((count,), jnp.int32).at[ranking[jnp.where(places < fixed, places, shifted)]].set(jnp.asarray(lengths, jnp.int32))

    lengths = jnp.where(number % 4 == 0, named(crowded, number // 4), named(ordinary, number - number // 4 - 1))
    mixed = jax.random.permutation(jax.random.fold_in(own, 3), count)
    source_of, taker = mixed[0:count // 2 * 2:2], mixed[1:count // 2 * 2:2]
    room = jnp.minimum(lengths[source_of] - 1, limit - lengths[taker]) // 2
    room = jnp.where((source_of == ranking[0]) | (taker == ranking[0]) | (lengths[taker] == 0), 0, jnp.maximum(room, 0))
    shifted = jax.random.randint(jax.random.fold_in(own, 4), (count // 2,), 0, 1 << 20) % (room + 1)
    lengths = lengths.at[source_of].add(-shifted).at[taker].add(shifted)
    items = jnp.searchsorted(jnp.cumsum(lengths), jnp.arange(rows * top), side="right").astype(jnp.int32)
    listing = items.reshape(top, rows).T
    listing = listing[jax.random.permutation(jax.random.fold_in(own, 1), rows)]
    offset_by = jax.random.randint(jax.random.fold_in(own, 2), (rows, 1), 0, top)
    return jnp.take_along_axis(listing, (jnp.arange(top)[None, :] + offset_by) % top, axis=1)


def shares(number_of, total, bound, skew, full):
    weights = [(1 << 20) // math.isqrt(standing ** skew) + 1 for standing in range(1, number_of + 1)]
    largest = bound if full else min(bound, max(-(-total // number_of), total * weights[0] // sum(weights)))
    least = 1 if total - largest >= number_of - 1 else 0
    counts, spare = [largest] + [least] * (number_of - 1), total - largest - least * (number_of - 1)
    while spare > 0:
        movable = [i for i in range(1, number_of) if counts[i] < largest] or [i for i in range(1, number_of) if counts[i] < bound]
        whole, left = sum([weights[i] for i in movable]), spare
        for i in movable:
            addition = min(bound - counts[i], max(1, left * weights[i] // whole), spare)
            counts[i] = counts[i] + addition
            spare = spare - addition
    return np.array(counts)


def bell_draw(stream_key, dims, spread, reach, cuts=(), kind=jnp.bfloat16):
    entries = jax.random.normal(stream_key, dims, jnp.float32) * spread
    if len(cuts) > 0:
        entries = levels(stream_key, dims, cuts, -0.22, 0.18) * entries
    return jnp.clip(entries, min=-reach, max=reach).astype(kind)


def setup_inputs(seed: int = 0) -> dict:
    splits = jax.random.split(jax.random.key(seed), 12)
    queries = draw_queries(jax.random.fold_in(splits[11], 71), 0)
    keys = draw_keys(jax.random.fold_in(splits[11], 71), 0)
    values = draw_values(jax.random.fold_in(splits[11], 71), 0)
    key_offset = draw_key_offset(jax.random.fold_in(splits[11], 71), 0)
    rows = bell_draw(splits[4], (TOKENS_B, D), 1.0, 6.0, ((0, 8),))
    gain = jnp.clip(1.0 + 0.18 * jax.random.normal(splits[5], (D,), jnp.float32), 0.1, 1.9)
    gate_w = bell_draw(splits[6], (EXPERTS, D, FF), D ** -0.5, 0.125, ((0, 8), (2, 4)))
    up_w = bell_draw(splits[7], (EXPERTS, D, FF), D ** -0.5, 0.125, ((0, 8), (2, 4)))
    down_w = bell_draw(splits[8], (EXPERTS, FF, D), FF ** -0.5, 0.09375, ((0, 8), (1, 4)))
    expert_ids_keys = jax.random.split(jax.random.fold_in(splits[9], 1), TOKENS_B // TOK_B_DEV)
    expert_ids_turns = jax.random.permutation(jax.random.fold_in(splits[9], 3), TOKENS_B // TOK_B_DEV)
    expert_ids = jax.vmap(lambda own, number: deal_out(jax.random.fold_in(splits[9], 2), own, number, TOK_B_DEV, EXPERTS, TOP, CAP, 0))(expert_ids_keys, expert_ids_turns).reshape((TOKENS_B, TOP))
    route_weights = jnp.clip(0.2 + 0.8 * jax.random.uniform(splits[10], (TOKENS_B, TOP), jnp.float32) ** levels(splits[10], (TOKENS_B, TOP), ((0, 8),), -0.2, 0.2), 0.2, 1.0)
    return dict(queries=queries, keys=keys, values=values, key_offset=key_offset, rows=rows, gain=gain, gate_w=gate_w, up_w=up_w, down_w=down_w, expert_ids=expert_ids, route_weights=route_weights)


EPSILON = 1e-06

def stick_mixer(queries, keys, values, key_offset):
    blocks = SEQUENCE_TOKENS // TOK_A_DEV
    scale = HD ** (-0.5)
    query_all = queries.astype(jnp.float32).reshape(blocks, TOK_A_DEV, ATTENTION_HEADS, HD)
    key_all = keys.astype(jnp.float32).reshape(blocks, TOK_A_DEV, ATTENTION_HEADS, HD)
    value_all = values.astype(jnp.float32).reshape(blocks, TOK_A_DEV, ATTENTION_HEADS, HD)
    offset_all = key_offset.astype(jnp.float32).reshape(blocks, TOK_A_DEV, ATTENTION_HEADS)
    positions = jnp.arange(TOK_A_DEV, dtype=jnp.int32)
    results = []
    for query_block in range(blocks):
        query_here = query_all[query_block]
        query_pos = query_block * TOK_A_DEV + positions

        def one_block(key_block):
            key_here = lax.dynamic_index_in_dim(key_all, key_block, 0, keepdims=False)
            value_here = lax.dynamic_index_in_dim(value_all, key_block, 0, keepdims=False)
            offset_here = lax.dynamic_index_in_dim(offset_all, key_block, 0, keepdims=False)
            logits = jnp.einsum('qhd,khd->hqk', query_here, key_here) * scale + offset_here.T[:, None, :]
            key_pos = key_block * TOK_A_DEV + positions
            strict = key_pos[None, None, :] < query_pos[None, :, None]
            breaks = jnp.where(strict, jax.nn.log_sigmoid(-logits), 0.0)
            within = lax.cumsum(breaks, axis=2, reverse=True) - breaks
            local = jnp.where(strict, jnp.exp(jax.nn.log_sigmoid(logits) + within), 0.0).astype(jnp.bfloat16)
            local = lax.optimization_barrier(local).astype(jnp.float32)
            summed = jnp.einsum('hqk,khd->hqd', local, value_here)
            return (summed, lax.optimization_barrier(jnp.sum(breaks, axis=2)))
        sums, totals = lax.map(one_block, jnp.arange(query_block + 1, dtype=jnp.int32))
        later = lax.cumsum(totals, axis=0, reverse=True) - totals
        combined = jnp.einsum('bhq,bhqd->qhd', jnp.exp(later), sums, precision=lax.Precision.HIGHEST)
        results.append(combined.reshape(TOK_A_DEV, ATTENTION_HEADS * HD))
    return jnp.concatenate(results, axis=0).astype(jnp.bfloat16)

def routed_experts(rows, gain, gate_w, up_w, down_w, expert_ids, route_weights):
    blocks = TOKENS_B // TOK_B_DEV
    rows_float = rows.astype(jnp.float32)
    normed = rows_float * lax.rsqrt(lax.optimization_barrier(jnp.mean(rows_float * rows_float, axis=1, keepdims=True)) + EPSILON)
    normed = (normed * gain.astype(jnp.float32)[None, :]).astype(jnp.bfloat16)
    block_ids = expert_ids.reshape(blocks, TOK_B_DEV * TOP)
    onehot = (block_ids[:, :, None] == jnp.arange(EXPERTS, dtype=jnp.int32)[None, None, :]).astype(jnp.int32)
    ranked = lax.optimization_barrier(jnp.sum((jnp.cumsum(onehot, axis=1) - onehot) * onehot, axis=2))
    token_of = jnp.arange(TOK_B_DEV * TOP, dtype=jnp.int32) // TOP

    def fill_table(ids_here, rank_here, block_index):
        table = jnp.zeros((EXPERTS * CAP,), jnp.int32)
        return table.at[ids_here * CAP + rank_here].set(token_of + block_index * TOK_B_DEV)
    tables = jax.vmap(fill_table)(block_ids, ranked, jnp.arange(blocks, dtype=jnp.int32))
    tables = tables.reshape(blocks, EXPERTS, CAP).transpose(1, 0, 2)
    group_width = FF // N_TP

    def one_expert(args):
        table, weight_gate, weight_up, weight_down = args
        inputs = normed[table.reshape(-1)]
        gate_val = jnp.dot(inputs, weight_gate, preferred_element_type=jnp.float32)
        up_val = jnp.dot(inputs, weight_up, preferred_element_type=jnp.float32)
        hidden = (jax.nn.silu(gate_val) * up_val).astype(jnp.bfloat16)
        grouped = hidden.reshape(-1, N_TP, group_width).astype(jnp.float32)
        down_grouped = weight_down.reshape(N_TP, group_width, D).astype(jnp.float32)
        parts = jnp.einsum('rnf,nfd->nrd', grouped, down_grouped).astype(jnp.bfloat16)
        parts = lax.optimization_barrier(parts).astype(jnp.float32)
        return lax.optimization_barrier(jnp.sum(parts, axis=0)).astype(jnp.bfloat16)
    outputs = lax.map(one_expert, (tables, gate_w, up_w, down_w))
    flat = outputs.reshape(EXPERTS * blocks * CAP, D)
    block_of = jnp.arange(TOKENS_B * TOP, dtype=jnp.int32) // (TOK_B_DEV * TOP)
    slot_index = block_ids.reshape(-1) * (blocks * CAP) + block_of * CAP + ranked.reshape(-1)
    picked = flat[slot_index].astype(jnp.float32).reshape(TOKENS_B, TOP, D)
    return lax.optimization_barrier(jnp.sum(picked * route_weights.astype(jnp.float32)[:, :, None], axis=1)).astype(jnp.bfloat16)

def reference(queries, keys, values, key_offset, rows, gain, gate_w, up_w, down_w, expert_ids, route_weights):
    attended = stick_mixer(queries, keys, values, key_offset)
    mixed = routed_experts(rows, gain, gate_w, up_w, down_w, expert_ids, route_weights)
    return (attended, mixed)
```

```python
import jax
import jax.numpy as jnp
from jax import lax
from jax.experimental import pallas as pl
from jax.experimental.pallas import tpu as pltpu
from jax.sharding import PartitionSpec as P

EPSILON = 1e-06


def stick_kernel(place_ref, q_ref, k_ref, v_ref, offset_ref, out_ref):
    rows, head_dim = q_ref.shape
    scale = head_dim ** (-0.5)
    place = place_ref[0]
    across = lax.broadcasted_iota(jnp.int32, (rows, rows), 0)
    along = lax.broadcasted_iota(jnp.int32, (rows, rows), 1)
    strict = along < across
    after = jnp.where(strict, 1.0, 0.0).astype(jnp.bfloat16)
    query = q_ref[...]

    def one_block(block, masked):
        here = pl.ds(pl.multiple_of(block * rows, rows), rows)
        logits = lax.dot_general(
            query, k_ref[here, :], (((1,), (1,)), ((), ())), preferred_element_type=jnp.float32
        )
        logits = logits * scale + offset_ref[0, pl.ds(block, 1), :]
        breaks = -(jnp.maximum(logits, 0.0) + jnp.log(1.0 + jnp.exp(-jnp.abs(logits))))
        chosen = logits + breaks
        if masked:
            breaks = jnp.where(strict, breaks, 0.0)
        within = jnp.dot(breaks.astype(jnp.bfloat16), after, preferred_element_type=jnp.float32)
        local = jnp.exp(chosen + within)
        if masked:
            local = jnp.where(strict, local, 0.0)
        summed = jnp.dot(
            local.astype(jnp.bfloat16), v_ref[here, :], preferred_element_type=jnp.float32
        )
        return summed, jnp.sum(breaks, axis=1, keepdims=True)

    def step(index, carry):
        total, later = carry
        summed, block_total = one_block(place - 1 - index, False)
        return total + jnp.exp(later) * summed, later + block_total

    total, _ = lax.fori_loop(0, place, step, one_block(place, True))
    out_ref[...] = total.astype(out_ref.dtype)


def stick_mixer(queries, keys, values, key_offset):
    query_len, width = queries.shape
    heads = key_offset.shape[1]
    head_dim = width // heads
    key_all = lax.all_gather(keys, "ep", axis=0, tiled=True)
    value_all = lax.all_gather(values, "ep", axis=0, tiled=True)
    offset_all = lax.all_gather(key_offset.T, "ep", axis=0)
    offset_all = jnp.swapaxes(offset_all, 0, 1).astype(jnp.float32)
    blocks = offset_all.shape[1]
    length = blocks * query_len
    place = lax.axis_index("ep").astype(jnp.int32).reshape(1)
    pairs = heads * blocks * query_len * query_len
    return pl.pallas_call(
        stick_kernel,
        grid=(heads,),
        in_specs=[
            pl.BlockSpec(memory_space=pltpu.SMEM),
            pl.BlockSpec((query_len, head_dim), lambda h: (0, h)),
            pl.BlockSpec((length, head_dim), lambda h: (0, h)),
            pl.BlockSpec((length, head_dim), lambda h: (0, h)),
            pl.BlockSpec((1, blocks, query_len), lambda h: (h, 0, 0)),
        ],
        out_specs=pl.BlockSpec((query_len, head_dim), lambda h: (0, h)),
        out_shape=jax.ShapeDtypeStruct((query_len, width), jnp.bfloat16),
        compiler_params=pltpu.CompilerParams(vmem_limit_bytes=40 * 1024 * 1024),
        cost_estimate=pl.CostEstimate(
            flops=pairs * 2 * (2 * head_dim + query_len),
            bytes_accessed=4 * length * width,
            transcendentals=3 * pairs,
        ),
        name="stick",
    )(place, queries, key_all, value_all, offset_all)


def routed_experts(rows, gain, gate_w, up_w, down_w, expert_ids, route_weights):
    ep_count = lax.axis_size("ep")
    tp_count = lax.axis_size("tp")
    local_experts = gate_w.shape[0]
    experts_all = ep_count * local_experts
    token_count = rows.shape[0]
    choose_count = expert_ids.shape[1]
    width = rows.shape[1]
    capacity = 2 * choose_count * token_count // experts_all
    part = capacity // tp_count
    rows_float = rows.astype(jnp.float32)
    normed = rows_float * lax.rsqrt(
        jnp.mean(rows_float * rows_float, axis=1, keepdims=True) + EPSILON
    )
    normed = (normed * gain[None, :]).astype(jnp.bfloat16)
    flat_ids = expert_ids.reshape(-1)
    onehot = (flat_ids[:, None] == jnp.arange(experts_all, dtype=jnp.int32)[None, :]).astype(
        jnp.int32
    )
    ranked = jnp.sum((jnp.cumsum(onehot, axis=0) - onehot) * onehot, axis=1)
    slot_index = flat_ids * capacity + ranked
    mine = lax.axis_index("tp") * part + jnp.arange(part, dtype=jnp.int32)
    wanted = (jnp.arange(experts_all, dtype=jnp.int32)[:, None] * capacity + mine).reshape(-1)
    pick = jnp.sum(
        (wanted[:, None, None] == slot_index.reshape(1, token_count, choose_count)), axis=2
    ).astype(jnp.bfloat16)
    outgoing = jnp.dot(pick, normed, preferred_element_type=jnp.float32).astype(jnp.bfloat16)
    outgoing = outgoing.reshape(ep_count, local_experts * part, width)
    arrived = lax.all_to_all(outgoing, "ep", split_axis=0, concat_axis=0, tiled=True)
    slots = lax.all_gather(arrived, "tp", axis=0)
    slots = slots.reshape(tp_count * ep_count, local_experts, part, width)
    slots = jnp.swapaxes(slots, 0, 1).reshape(local_experts, -1, width)
    gate_val = jnp.einsum("xnd,xdf->xnf", slots, gate_w, preferred_element_type=jnp.float32)
    up_val = jnp.einsum("xnd,xdf->xnf", slots, up_w, preferred_element_type=jnp.float32)
    hidden = (jax.nn.silu(gate_val) * up_val).astype(jnp.bfloat16)
    parts = jnp.einsum("xnf,xfd->xnd", hidden, down_w, preferred_element_type=jnp.float32).astype(
        jnp.bfloat16
    )
    share = lax.psum_scatter(parts, "tp", scatter_dimension=2, tiled=True)
    share = share.reshape(local_experts, tp_count, ep_count, part, width // tp_count)
    returned = lax.all_to_all(share, "ep", split_axis=2, concat_axis=0, tiled=True)
    flat_out = returned.reshape(experts_all * capacity, width // tp_count)
    picked = flat_out[slot_index].astype(jnp.float32)
    picked = picked.reshape(token_count, choose_count, width // tp_count)
    mixed = jnp.sum(picked * route_weights[:, :, None], axis=1).astype(jnp.bfloat16)
    return lax.all_gather(mixed, "tp", axis=1, tiled=True)


def body(
    queries, keys, values, key_offset, rows, gain, gate_w, up_w, down_w, expert_ids, route_weights
):
    attended = stick_mixer(queries, keys, values, key_offset)
    mixed = routed_experts(rows, gain, gate_w, up_w, down_w, expert_ids, route_weights)
    return (attended, mixed)


def solution(mesh):
    in_specs = (
        P("ep", "tp"),
        P("ep", "tp"),
        P("ep", "tp"),
        P("ep", "tp"),
        P("ep", None),
        P(),
        P("ep", None, "tp"),
        P("ep", None, "tp"),
        P("ep", "tp", None),
        P("ep", None),
        P("ep", None),
    )
    out_specs = (P("ep", "tp"), P("ep", None))
    return jax.shard_map(body, mesh=mesh, in_specs=in_specs, out_specs=out_specs, check_vma=False)
```

```python
import jax
import jax.numpy as jnp
from jax import lax
from jax.experimental import pallas as pl
from jax.experimental.pallas import tpu as pltpu
from jax.sharding import PartitionSpec as P

EPSILON = 1e-06


def stick_kernel(
    place_ref, q_ref, other_ref, k_ref, v_ref, offset_ref, total_ref, decay_ref, partial_ref
):
    rows, head_dim = q_ref.shape
    scale = head_dim ** (-0.5)
    place, others = place_ref[0], place_ref[1]
    across = lax.broadcasted_iota(jnp.int32, (rows, rows), 0)
    along = lax.broadcasted_iota(jnp.int32, (rows, rows), 1)
    strict = along < across
    after = jnp.where(strict, 1.0, 0.0).astype(jnp.bfloat16)

    def one_block(query, block, masked):
        here = pl.ds(pl.multiple_of(block * rows, rows), rows)
        logits = lax.dot_general(
            query, k_ref[here, :], (((1,), (1,)), ((), ())), preferred_element_type=jnp.float32
        )
        logits = logits * scale + offset_ref[0, pl.ds(block, 1), :]
        breaks = -(jnp.maximum(logits, 0.0) + jnp.log(1.0 + jnp.exp(-jnp.abs(logits))))
        chosen = logits + breaks
        if masked:
            breaks = jnp.where(strict, breaks, 0.0)
        within = jnp.dot(breaks.astype(jnp.bfloat16), after, preferred_element_type=jnp.float32)
        local = jnp.exp(chosen + within)
        if masked:
            local = jnp.where(strict, local, 0.0)
        summed = jnp.dot(
            local.astype(jnp.bfloat16), v_ref[here, :], preferred_element_type=jnp.float32
        )
        return summed, jnp.sum(breaks, axis=1, keepdims=True)

    def walk(query, count, start):
        def step(index, carry):
            total, later = carry
            summed, block_total = one_block(query, count - 1 - index, False)
            return total + jnp.exp(later) * summed, later + block_total

        return lax.fori_loop(0, count, step, start)

    query = q_ref[...]
    total, later = walk(query, place, one_block(query, place, True))
    total_ref[...] = total
    decay_ref[...] = jnp.broadcast_to(jnp.exp(later), total.shape)
    nothing = (jnp.zeros((rows, head_dim), jnp.float32), jnp.zeros((rows, 1), jnp.float32))
    partial, _ = walk(other_ref[...], others, nothing)
    partial_ref[...] = partial.astype(partial_ref.dtype)


def halves():
    count = lax.axis_size("ep")
    half = count // 2
    return half, [list(range(half)), list(range(half, count))]


def gather_half(array, axis, tiled):
    return lax.all_gather(array, "ep", axis=axis, tiled=tiled, axis_index_groups=halves()[1])


def attend(queries, others, key_half, value_half, offset_half):
    query_len, width = queries.shape
    heads, blocks = offset_half.shape[:2]
    head_dim = width // heads
    length = blocks * query_len
    position = lax.axis_index("ep").astype(jnp.int32)
    place = jnp.stack([position % blocks, jnp.where(position < blocks, blocks, 0)])
    pairs = 2 * heads * blocks * query_len * query_len
    one = pl.BlockSpec((query_len, head_dim), lambda h: (0, h))
    whole = pl.BlockSpec((length, head_dim), lambda h: (0, h))
    return pl.pallas_call(
        stick_kernel,
        grid=(heads,),
        in_specs=[
            pl.BlockSpec(memory_space=pltpu.SMEM),
            one,
            one,
            whole,
            whole,
            pl.BlockSpec((1, blocks, query_len), lambda h: (h, 0, 0)),
        ],
        out_specs=[one, one, one],
        out_shape=[
            jax.ShapeDtypeStruct((query_len, width), jnp.float32),
            jax.ShapeDtypeStruct((query_len, width), jnp.float32),
            jax.ShapeDtypeStruct((query_len, width), jnp.bfloat16),
        ],
        compiler_params=pltpu.CompilerParams(vmem_limit_bytes=40 * 1024 * 1024),
        cost_estimate=pl.CostEstimate(
            flops=pairs * 2 * (2 * head_dim + query_len),
            bytes_accessed=4 * length * width,
            transcendentals=3 * pairs,
        ),
        name="stick",
    )(place, queries, others, key_half, value_half, offset_half)


def layer(
    queries, keys, values, key_offset, rows, gain, gate_w, up_w, down_w, expert_ids, route_weights
):
    half = halves()[0]
    offset_half = gather_half(key_offset.T, 0, False)
    rows, offset_half = lax.optimization_barrier((rows, offset_half))
    offset_half = jnp.swapaxes(offset_half, 0, 1).astype(jnp.float32)
    value_half = gather_half(values, 0, True)
    others = lax.ppermute(queries, "ep", [(half + i, i) for i in range(half)])
    ep_count = lax.axis_size("ep")
    tp_count = lax.axis_size("tp")
    local_experts = gate_w.shape[0]
    experts_all = ep_count * local_experts
    token_count = rows.shape[0]
    choose_count = expert_ids.shape[1]
    width = rows.shape[1]
    capacity = 2 * choose_count * token_count // experts_all
    part = capacity // tp_count
    rows_float = rows.astype(jnp.float32)
    normed = rows_float * lax.rsqrt(
        jnp.mean(rows_float * rows_float, axis=1, keepdims=True) + EPSILON
    )
    normed = (normed * gain[None, :]).astype(jnp.bfloat16)
    flat_ids = expert_ids.reshape(-1)
    onehot = (flat_ids[:, None] == jnp.arange(experts_all, dtype=jnp.int32)[None, :]).astype(
        jnp.int32
    )
    ranked = jnp.sum((jnp.cumsum(onehot, axis=0) - onehot) * onehot, axis=1)
    slot_index = flat_ids * capacity + ranked
    mine = lax.axis_index("tp") * part + jnp.arange(part, dtype=jnp.int32)
    wanted = (jnp.arange(experts_all, dtype=jnp.int32)[:, None] * capacity + mine).reshape(-1)
    pick = jnp.sum(
        (wanted[:, None, None] == slot_index.reshape(1, token_count, choose_count)), axis=2
    ).astype(jnp.bfloat16)
    outgoing = jnp.dot(pick, normed, preferred_element_type=jnp.float32).astype(jnp.bfloat16)
    outgoing = outgoing.reshape(ep_count, local_experts * part, width)
    arrived = lax.all_to_all(outgoing, "ep", split_axis=0, concat_axis=0, tiled=True)
    arrived, value_half, others = lax.optimization_barrier((arrived, value_half, others))
    slots = lax.all_gather(arrived, "tp", axis=0)
    slots, keys = lax.optimization_barrier((slots, keys))
    key_half = gather_half(keys, 0, True)
    slots = slots.reshape(tp_count * ep_count, local_experts, part, width)
    slots = jnp.swapaxes(slots, 0, 1).reshape(local_experts, -1, width)
    gate_val = jnp.einsum("xnd,xdf->xnf", slots, gate_w, preferred_element_type=jnp.float32)
    up_val = jnp.einsum("xnd,xdf->xnf", slots, up_w, preferred_element_type=jnp.float32)
    hidden = (jax.nn.silu(gate_val) * up_val).astype(jnp.bfloat16)
    parts = jnp.einsum("xnf,xfd->xnd", hidden, down_w, preferred_element_type=jnp.float32).astype(
        jnp.bfloat16
    )
    parts, key_half, value_half = lax.optimization_barrier((parts, key_half, value_half))
    total, decay, partial = attend(queries, others, key_half, value_half, offset_half)
    share = lax.psum_scatter(parts, "tp", scatter_dimension=2, tiled=True)
    share, partial = lax.optimization_barrier((share, partial))
    early = lax.ppermute(partial, "ep", [(i, half + i) for i in range(half)])
    attended = (total + decay * early.astype(jnp.float32)).astype(jnp.bfloat16)
    share = share.reshape(local_experts, tp_count, ep_count, part, width // tp_count)
    returned = lax.all_to_all(share, "ep", split_axis=2, concat_axis=0, tiled=True)
    flat_out = returned.reshape(experts_all * capacity, width // tp_count)
    picked = flat_out[slot_index].astype(jnp.float32)
    picked = picked.reshape(token_count, choose_count, width // tp_count)
    mixed = jnp.sum(picked * route_weights[:, :, None], axis=1).astype(jnp.bfloat16)
    return attended, lax.all_gather(mixed, "tp", axis=1, tiled=True)


def solution(mesh):
    in_specs = (
        P("ep", "tp"),
        P("ep", "tp"),
        P("ep", "tp"),
        P("ep", "tp"),
        P("ep", None),
        P(),
        P("ep", None, "tp"),
        P("ep", None, "tp"),
        P("ep", "tp", None),
        P("ep", None),
        P("ep", None),
    )
    out_specs = (P("ep", "tp"), P("ep", None))
    return jax.shard_map(layer, mesh=mesh, in_specs=in_specs, out_specs=out_specs, check_vma=False)
```

```python
import jax
import jax.numpy as jnp
from jax import lax
from jax.experimental import pallas as pl
from jax.experimental.pallas import tpu as pltpu
from jax.sharding import PartitionSpec as P

EPSILON = 1e-06


def stick_kernel(
    place_ref, q_ref, other_ref, k_ref, v_ref, offset_ref, total_ref, decay_ref, partial_ref
):
    rows, head_dim = q_ref.shape
    scale = head_dim ** (-0.5)
    place, others = place_ref[0], place_ref[1]
    across = lax.broadcasted_iota(jnp.int32, (rows, rows), 0)
    along = lax.broadcasted_iota(jnp.int32, (rows, rows), 1)
    strict = along < across
    after = jnp.where(strict, 1.0, 0.0).astype(jnp.bfloat16)

    def one_block(query, block, masked):
        here = pl.ds(pl.multiple_of(block * rows, rows), rows)
        logits = lax.dot_general(
            query, k_ref[here, :], (((1,), (1,)), ((), ())), preferred_element_type=jnp.float32
        )
        logits = logits * scale + offset_ref[0, pl.ds(block, 1), :]
        breaks = -(jnp.maximum(logits, 0.0) + jnp.log(1.0 + jnp.exp(-jnp.abs(logits))))
        chosen = logits + breaks
        if masked:
            breaks = jnp.where(strict, breaks, 0.0)
        within = jnp.dot(breaks.astype(jnp.bfloat16), after, preferred_element_type=jnp.float32)
        local = jnp.exp(chosen + within)
        if masked:
            local = jnp.where(strict, local, 0.0)
        summed = jnp.dot(
            local.astype(jnp.bfloat16), v_ref[here, :], preferred_element_type=jnp.float32
        )
        return summed, jnp.sum(breaks, axis=1, keepdims=True)

    def walk(query, count, start):
        def step(index, carry):
            total, later = carry
            summed, block_total = one_block(query, count - 1 - index, False)
            return total + jnp.exp(later) * summed, later + block_total

        return lax.fori_loop(0, count, step, start)

    query = q_ref[...]
    total, later = walk(query, place, one_block(query, place, True))
    total_ref[...] = total
    decay_ref[...] = jnp.broadcast_to(jnp.exp(later), total.shape)
    nothing = (jnp.zeros((rows, head_dim), jnp.float32), jnp.zeros((rows, 1), jnp.float32))
    partial, _ = walk(other_ref[...], others, nothing)
    partial_ref[...] = partial.astype(partial_ref.dtype)


def halves():
    count = lax.axis_size("ep")
    half = count // 2
    return half, [list(range(half)), list(range(half, count))]


def gather_half(array, axis, tiled):
    return lax.all_gather(array, "ep", axis=axis, tiled=tiled, axis_index_groups=halves()[1])


def attend(queries, others, key_half, value_half, offset_half):
    query_len, width = queries.shape
    heads, blocks = offset_half.shape[:2]
    head_dim = width // heads
    length = blocks * query_len
    position = lax.axis_index("ep").astype(jnp.int32)
    place = jnp.stack([position % blocks, jnp.where(position < blocks, blocks, 0)])
    pairs = 2 * heads * blocks * query_len * query_len
    one = pl.BlockSpec((query_len, head_dim), lambda h: (0, h))
    whole = pl.BlockSpec((length, head_dim), lambda h: (0, h))
    return pl.pallas_call(
        stick_kernel,
        grid=(heads,),
        in_specs=[
            pl.BlockSpec(memory_space=pltpu.SMEM),
            one,
            one,
            whole,
            whole,
            pl.BlockSpec((1, blocks, query_len), lambda h: (h, 0, 0)),
        ],
        out_specs=[one, one, one],
        out_shape=[
            jax.ShapeDtypeStruct((query_len, width), jnp.float32),
            jax.ShapeDtypeStruct((query_len, width), jnp.float32),
            jax.ShapeDtypeStruct((query_len, width), jnp.bfloat16),
        ],
        compiler_params=pltpu.CompilerParams(vmem_limit_bytes=40 * 1024 * 1024),
        cost_estimate=pl.CostEstimate(
            flops=pairs * 2 * (2 * head_dim + query_len),
            bytes_accessed=4 * length * width,
            transcendentals=3 * pairs,
        ),
        name="stick",
    )(place, queries, others, key_half, value_half, offset_half)


def layer(
    queries, keys, values, key_offset, rows, gain, gate_w, up_w, down_w, expert_ids, route_weights
):
    half = halves()[0]
    offset_half = gather_half(key_offset.T, 0, False)
    rows, offset_half = lax.optimization_barrier((rows, offset_half))
    offset_half = jnp.swapaxes(offset_half, 0, 1).astype(jnp.float32)
    key_half = gather_half(keys, 0, True)
    value_half = gather_half(values, 0, True)
    others = lax.ppermute(queries, "ep", [(half + i, i) for i in range(half)])
    ep_count = lax.axis_size("ep")
    tp_count = lax.axis_size("tp")
    local_experts = gate_w.shape[0]
    experts_all = ep_count * local_experts
    token_count = rows.shape[0]
    choose_count = expert_ids.shape[1]
    width = rows.shape[1]
    capacity = 2 * choose_count * token_count // experts_all
    part = capacity // tp_count
    rows_float = rows.astype(jnp.float32)
    normed = rows_float * lax.rsqrt(
        jnp.mean(rows_float * rows_float, axis=1, keepdims=True) + EPSILON
    )
    normed = (normed * gain[None, :]).astype(jnp.bfloat16)
    flat_ids = expert_ids.reshape(-1)
    onehot = (flat_ids[:, None] == jnp.arange(experts_all, dtype=jnp.int32)[None, :]).astype(
        jnp.int32
    )
    ranked = jnp.sum((jnp.cumsum(onehot, axis=0) - onehot) * onehot, axis=1)
    slot_index = flat_ids * capacity + ranked
    mine = lax.axis_index("tp") * part + jnp.arange(part, dtype=jnp.int32)
    wanted = (jnp.arange(experts_all, dtype=jnp.int32)[:, None] * capacity + mine).reshape(-1)
    pick = jnp.sum(
        (wanted[:, None, None] == slot_index.reshape(1, token_count, choose_count)), axis=2
    ).astype(jnp.bfloat16)
    outgoing = jnp.dot(pick, normed, preferred_element_type=jnp.float32).astype(jnp.bfloat16)
    outgoing = outgoing.reshape(ep_count, local_experts * part, width)
    arrived = lax.all_to_all(outgoing, "ep", split_axis=0, concat_axis=0, tiled=True)
    arrived, key_half, value_half, others = lax.optimization_barrier(
        (arrived, key_half, value_half, others)
    )
    slots = lax.all_gather(arrived, "tp", axis=0)
    total, decay, partial = attend(queries, others, key_half, value_half, offset_half)
    slots, partial = lax.optimization_barrier((slots, partial))
    early = lax.ppermute(partial, "ep", [(i, half + i) for i in range(half)])
    slots = slots.reshape(tp_count * ep_count, local_experts, part, width)
    slots = jnp.swapaxes(slots, 0, 1).reshape(local_experts, -1, width)
    gate_val = jnp.einsum("xnd,xdf->xnf", slots, gate_w, preferred_element_type=jnp.float32)
    up_val = jnp.einsum("xnd,xdf->xnf", slots, up_w, preferred_element_type=jnp.float32)
    hidden = (jax.nn.silu(gate_val) * up_val).astype(jnp.bfloat16)
    parts = jnp.einsum("xnf,xfd->xnd", hidden, down_w, preferred_element_type=jnp.float32).astype(
        jnp.bfloat16
    )
    share = lax.psum_scatter(parts, "tp", scatter_dimension=2, tiled=True)
    share, early = lax.optimization_barrier((share, early))
    attended = (total + decay * early.astype(jnp.float32)).astype(jnp.bfloat16)
    share = share.reshape(local_experts, tp_count, ep_count, part, width // tp_count)
    returned = lax.all_to_all(share, "ep", split_axis=2, concat_axis=0, tiled=True)
    flat_out = returned.reshape(experts_all * capacity, width // tp_count)
    picked = flat_out[slot_index].astype(jnp.float32)
    picked = picked.reshape(token_count, choose_count, width // tp_count)
    mixed = jnp.sum(picked * route_weights[:, :, None], axis=1).astype(jnp.bfloat16)
    return attended, lax.all_gather(mixed, "tp", axis=1, tiled=True)


def solution(mesh):
    in_specs = (
        P("ep", "tp"),
        P("ep", "tp"),
        P("ep", "tp"),
        P("ep", "tp"),
        P("ep", None),
        P(),
        P("ep", None, "tp"),
        P("ep", None, "tp"),
        P("ep", "tp", None),
        P("ep", None),
        P("ep", None),
    )
    out_specs = (P("ep", "tp"), P("ep", None))
    return jax.shard_map(layer, mesh=mesh, in_specs=in_specs, out_specs=out_specs, check_vma=False)
```
